32 devices in a mesh: ep: 32 (over z, y, x, core).
Axes of the slice: x: 2, y: 2, z: 4, core: 2. Of those that a mesh axis runs over, the one named last changes fastest.
Arguments:
- tokens: bfloat16 [256, 2048], P('ep'), may hold values from -6 to 6
- cache_keys: bfloat16 [256, 1024, 128], P('ep'), may hold values from -80 to 80
- cache_values: bfloat16 [256, 1024, 128], P('ep'), may hold values from -6 to 6
- cum_gates: float32 [256, 1024, 2], P('ep'), may hold values from -1024 to 0, as said below
- lengths: int32 [256], P('ep'), may hold values from 128 to 1024
- query_weight: bfloat16 [2048, 2048], replicated, may hold values from -0.125 to 0.125
- key_weight: bfloat16 [2048, 128], replicated, may hold values from -0.125 to 0.125
- value_weight: bfloat16 [2048, 128], replicated, may hold values from -0.125 to 0.125
- forget_weight: bfloat16 [2048, 2], replicated, may hold values from -0.125 to 0.125
- out_weight: bfloat16 [2048, 2048], P('ep'), may hold values from -1 to 1
- norm_gain: float32 [2, 2048], replicated, may hold values from 0.1 to 1.9
- norm_bias: float32 [2, 2048], replicated, may hold values from -1 to 1
- dense_gate_weight: bfloat16 [2048, 5632], P(None, 'ep'), may hold values from -0.125 to 0.125
- dense_up_weight: bfloat16 [2048, 5632], P(None, 'ep'), may hold values from -0.125 to 0.125
- dense_down_weight: bfloat16 [5632, 2048], P('ep'), may hold values from -0.078125 to 0.078125
- dense_scale: float32 [2048], replicated, may hold values from 0.2 to 1.5
- expert_gate_weight: bfloat16 [2048, 57344], P(None, 'ep'), may hold values from -0.125 to 0.125
- expert_up_weight: bfloat16 [2048, 57344], P(None, 'ep'), may hold values from -0.125 to 0.125
- expert_down_weight: bfloat16 [57344, 2048], P('ep'), may hold values from -0.0625 to 0.0625
- routes: int32 [256, 2], replicated, may hold values from 0 to 7, all different within a row; in each aligned block of 8 rows (0 to 7, 8 to 15, ...) at most 3 rows name the same one
- route_weights: float32 [256, 2], replicated, may hold values from 0.2 to 1
Outputs:
- output: bfloat16 [256, 2048], P('ep')
The draws below stay inside these ranges and needn't reach their ends.
Inputs may be any that keep to these rules, and one draw needn't show every extreme that they name: `routes`: each row names 2 different experts; the rows of one device (8 aligned rows) name one expert at most 3 times. `cum_gates`: non-increasing along positions.
All inputs are finite; a program needn't handle non-finite values.
Results may differ from the reference program's by a relative error of at most 0.012.
Values may be sent and summed in bfloat16 or wider, within the bound.
A program may use at most 128 MiB of HBM per device.

```python
import math
import jax
import jax.numpy as jnp
import numpy as np
from jax import lax

D = 2048
HEADS = 32
HEAD_DIM = 64
KEY_VALUE_HEADS = 2
FF_DENSE = 5632
FF_EXPERT = 7168
EXPERTS = 8
TOP = 2
SEQ_DEV = 8
CACHE_SLOTS = 1024
SEQUENCE_COUNT = 256
CAP = 3
N_EP = 32


def draw_cache_keys(key, part):
    key_rows = jax.random.split(key, 1)
    shape = (SEQUENCE_COUNT, CACHE_SLOTS, KEY_VALUE_HEADS * HEAD_DIM)
    return jax.random.normal(key_rows[0], shape, jnp.float32).astype(jnp.bfloat16)


def draw_cum_gates(key, part):
    key_rows = jax.random.split(key, 7)
    devices = SEQUENCE_COUNT // SEQ_DEV
    share_fast = 0.5
    fast = jax.random.uniform(key_rows[0], (SEQUENCE_COUNT, 1, KEY_VALUE_HEADS)) < share_fast
    fast_rate = jnp.exp(jax.random.uniform(key_rows[1], (SEQUENCE_COUNT, 1, KEY_VALUE_HEADS), jnp.float32, math.log(1.0 / 100.0), math.log(1.0 / 30.0)))
    slow_rate = jnp.exp(jax.random.uniform(key_rows[2], (SEQUENCE_COUNT, 1, KEY_VALUE_HEADS), jnp.float32, math.log(0.1), math.log(0.4))) / CACHE_SLOTS
    decay_rate = jnp.where(fast, fast_rate, slow_rate)
    per_device_ratio = jnp.exp(jax.random.uniform(key_rows[3], (devices, 1, 1), jnp.float32, 0.0, math.log(3.0)))
    per_device_ratio = jnp.repeat(per_device_ratio, SEQ_DEV, axis=0)
    coarse_estimate = jnp.exp(jax.random.uniform(key_rows[4], (SEQUENCE_COUNT, CACHE_SLOTS, KEY_VALUE_HEADS), jnp.float32, math.log(0.5), math.log(2.0)))
    spike_position = jax.random.randint(key_rows[5], (SEQUENCE_COUNT, 1, KEY_VALUE_HEADS, 2), 0, CACHE_SLOTS)
    decay_penalty = jax.random.uniform(key_rows[6], (SEQUENCE_COUNT, 1, KEY_VALUE_HEADS, 2), jnp.float32, 0.2, 0.5)
    current_slot = jnp.arange(CACHE_SLOTS, dtype=jnp.int32)[None, :, None, None]
    spike_amount = jnp.sum(jnp.where(current_slot == spike_position, -jnp.log(1.0 - decay_penalty), 0.0), axis=3)
    step_total = decay_rate * per_device_ratio * coarse_estimate + spike_amount
    return jnp.cumsum(-step_total, axis=1).astype(jnp.float32)


def with_ends(result, key, least, largest):
    longest = result.shape.index(max(result.shape))
    spots = []
    for shift in (0, 1):
        where = [jax.random.randint(jax.random.fold_in(key, axis), (), 0, length) for axis, length in enumerate(result.shape)]
        where[longest] = (where[longest] + shift) % result.shape[longest]
        spots.append(tuple(where))
    return result.at[spots[0]].set(least).at[spots[1]].set(largest)


def levels(stream_key, dims, cuts, smallest, top_value):
    level, own = 1.0, jax.random.fold_in(stream_key, 6)
    for dim, parts in cuts:
        heights = jnp.exp(jax.random.uniform(jax.random.fold_in(own, dim), (parts,), jnp.float32, smallest / len(cuts), top_value / len(cuts)))
        level = level * jnp.repeat(heights, dims[dim] // parts).reshape([-1 if axis == dim else 1 for axis in range(len(dims))])
    return level


def routed_block(stream_key, own, number, rows, count, top, reach, slope):
    ranking = jax.random.permutation(stream_key, count)
    crowded, common = load_shares(count, rows * top, reach, slope, True), load_shares(count, rows * top, reach, slope, False)
    places = jnp.arange(count)

    def named(tallies, turn):
        used = int((tallies > 0).sum())
        fixed = max(1, used // 4)
        shifted = fixed + (places - fixed + turn * (used - fixed)) % max(1, count - fixed)
        return jnp.zeros((count,), jnp.int32).at[ranking[jnp.where(places < fixed, places, shifted)]].set(jnp.asarray(tallies, jnp.int32))

    tallies = jnp.where(number % 4 == 0, named(crowded, number // 4), named(common, number - number // 4 - 1))
    mixed = jax.random.permutation(jax.random.fold_in(own, 3), count)
    source_of, taker = mixed[0:count // 2 * 2:2], mixed[1:count // 2 * 2:2]
    slack = jnp.minimum(tallies[source_of] - 1, reach - tallies[taker]) // 2
    slack = jnp.where((source_of == ranking[0]) | (taker == ranking[0]) | (tallies[taker] == 0), 0, jnp.maximum(slack, 0))
    shifted = jax.random.randint(jax.random.fold_in(own, 4), (count // 2,), 0, 1 << 20) % (slack + 1)
    tallies = tallies.at[source_of].add(-shifted).at[taker].add(shifted)
    items = jnp.searchsorted(jnp.cumsum(tallies), jnp.arange(rows * top), side="right").astype(jnp.int32)
    table = items.reshape(top, rows).T
    table = table[jax.random.permutation(jax.random.fold_in(own, 1), rows)]
    turn = jax.random.randint(jax.random.fold_in(own, 2), (rows, 1), 0, top)
    return jnp.take_along_axis(table, (jnp.arange(top)[None, :] + turn) % top, axis=1)


def load_shares(count, total, bound, skew, full):
    weights = [(1 << 20) // math.isqrt(rank ** skew) + 1 for rank in range(1, count + 1)]
    largest = bound if full else min(bound, max(-(-total // count), total * weights[0] // sum(weights)))
    least = 1 if total - largest >= count - 1 else 0
    holding, spare = [largest] + [least] * (count - 1), total - largest - least * (count - 1)
    while spare > 0:
        movable = [i for i in range(1, count) if holding[i] < largest] or [i for i in range(1, count) if holding[i] < bound]
        whole, remaining = sum([weights[i] for i in movable]), spare
        for i in movable:
            more = min(bound - holding[i], max(1, remaining * weights[i] // whole), spare)
            holding[i] = holding[i] + more
            spare = spare - more
    return np.array(holding)


def normal_values(stream_key, shape, scale, reach, cuts=(), held_as=jnp.bfloat16):
    level = levels(stream_key, shape, cuts, -0.22, 0.18) if cuts else 1.0
    values = jax.random.normal(stream_key, shape, jnp.float32) * scale * level
    return jnp.minimum(jnp.maximum(values, -reach), reach).astype(held_as)


def setup_inputs(seed: int = 0) -> dict:
    keys = jax.random.split(jax.random.key(seed), 22)
    tokens = normal_values(keys[0], (SEQUENCE_COUNT, D), 1.0, 6.0, ((0, 32),))
    cache_keys = draw_cache_keys(jax.random.fold_in(keys[21], 71), 0)
    cache_values = normal_values(keys[2], (SEQUENCE_COUNT, CACHE_SLOTS, KEY_VALUE_HEADS * HEAD_DIM), 1.0, 6.0, ((0, 32),))
    cum_gates = draw_cum_gates(jax.random.fold_in(keys[21], 71), 0)
    lengths = with_ends(jax.random.randint(keys[4], (SEQUENCE_COUNT,), CACHE_SLOTS // 8, CACHE_SLOTS + 1), jax.random.fold_in(keys[4], 1), CACHE_SLOTS // 8, CACHE_SLOTS).astype(jnp.int32)
    query_weight = normal_values(keys[5], (D, HEADS * HEAD_DIM), D ** -0.5, 0.125)
    key_weight = normal_values(keys[6], (D, KEY_VALUE_HEADS * HEAD_DIM), D ** -0.5, 0.125)
    value_weight = normal_values(keys[7], (D, KEY_VALUE_HEADS * HEAD_DIM), D ** -0.5, 0.125)
    forget_weight = normal_values(keys[8], (D, KEY_VALUE_HEADS), D ** -0.5, 0.125)
    out_weight = normal_values(keys[9], (HEADS * HEAD_DIM, D), (HEADS * HEAD_DIM // 64) ** -0.5, 1.0, ((0, 32),))
    norm_gain = jnp.clip(1.0 + 0.18 * jax.random.normal(keys[10], (2, D), jnp.float32), 0.1, 1.9)
    norm_bias = normal_values(keys[11], (2, D), 0.2, 1.0, (), jnp.float32)
    dense_gate_weight = normal_values(keys[12], (D, FF_DENSE), D ** -0.5, 0.125, ((1, 32),))
    dense_up_weight = normal_values(keys[13], (D, FF_DENSE), D ** -0.5, 0.125, ((1, 32),))
    dense_down_weight = normal_values(keys[14], (FF_DENSE, D), FF_DENSE ** -0.5, 0.078125, ((0, 32),))
    dense_scale = jnp.clip(jax.random.uniform(keys[15], (D,), jnp.float32, 0.2, 1.5), 0.2, 1.5)
    expert_gate_weight = normal_values(keys[16], (D, EXPERTS * FF_EXPERT), D ** -0.5, 0.125, ((1, 32),))
    expert_up_weight = normal_values(keys[17], (D, EXPERTS * FF_EXPERT), D ** -0.5, 0.125, ((1, 32),))
    expert_down_weight = normal_values(keys[18], (EXPERTS * FF_EXPERT, D), FF_EXPERT ** -0.5, 0.0625, ((0, 32),))
    routes_keys = jax.random.split(jax.random.fold_in(keys[19], 1), SEQUENCE_COUNT // SEQ_DEV)
    routes_turns = jax.random.permutation(jax.random.fold_in(keys[19], 3), SEQUENCE_COUNT // SEQ_DEV)
    routes = jax.vmap(lambda own, number: routed_block(jax.random.fold_in(keys[19], 2), own, number, SEQ_DEV, EXPERTS, TOP, CAP, 2))(routes_keys, routes_turns).reshape((SEQUENCE_COUNT, TOP))
    route_weights = jnp.clip(jax.random.uniform(keys[20], (SEQUENCE_COUNT, TOP), jnp.float32, 0.2, 1.0), 0.2, 1.0)
    return dict(tokens=tokens, cache_keys=cache_keys, cache_values=cache_values, cum_gates=cum_gates, lengths=lengths, query_weight=query_weight, key_weight=key_weight, value_weight=value_weight, forget_weight=forget_weight, out_weight=out_weight, norm_gain=norm_gain, norm_bias=norm_bias, dense_gate_weight=dense_gate_weight, dense_up_weight=dense_up_weight, dense_down_weight=dense_down_weight, dense_scale=dense_scale, expert_gate_weight=expert_gate_weight, expert_up_weight=expert_up_weight, expert_down_weight=expert_down_weight, routes=routes, route_weights=route_weights)


residual_scale = 1.4142135
norm_eps = 1e-05

def layer_norm(values, gain_row, shift_row):
    centre = lax.optimization_barrier(jnp.mean(values, axis=-1, keepdims=True))
    centred = values - centre
    spread = lax.optimization_barrier(jnp.mean(centred * centred, axis=-1, keepdims=True))
    return (centred * lax.rsqrt(spread + norm_eps) * gain_row + shift_row).astype(jnp.bfloat16)

def attend_block(inputs):
    queries, cached_keys, cached_values, gate_sums, length_row, fresh_key, fresh_value, fresh_gate = inputs
    amount = queries.shape[0]
    grouped = HEADS // KEY_VALUE_HEADS
    query_grid_four = queries.astype(jnp.float32).reshape(amount, KEY_VALUE_HEADS, grouped, HEAD_DIM)
    key_four = cached_keys.astype(jnp.float32).reshape(amount, CACHE_SLOTS, KEY_VALUE_HEADS, HEAD_DIM)
    value_four = cached_values.astype(jnp.float32).reshape(amount, CACHE_SLOTS, KEY_VALUE_HEADS, HEAD_DIM)
    self_key_row = fresh_key.astype(jnp.float32).reshape(amount, KEY_VALUE_HEADS, HEAD_DIM)
    own_value = fresh_value.astype(jnp.float32).reshape(amount, KEY_VALUE_HEADS, HEAD_DIM)
    ratio_value = HEAD_DIM ** (-0.5)
    latest = jnp.take_along_axis(gate_sums, (length_row - 1).astype(jnp.int32)[:, None, None], axis=1)
    offsets = jnp.transpose(latest - gate_sums + fresh_gate[:, None, :], (0, 2, 1))
    past = jnp.einsum('bkgd,blkd->bkgl', query_grid_four, key_four) * ratio_value + offsets[:, :, None, :]
    live = jnp.arange(CACHE_SLOTS, dtype=jnp.int32)[None, :] < length_row[:, None]
    past = jnp.where(live[:, None, None, :], past, -jnp.inf)
    self_part = jnp.einsum('rifs,ris->rif', query_grid_four, self_key_row) * ratio_value
    highest = jnp.maximum(lax.optimization_barrier(jnp.max(past, axis=-1)), self_part)
    past_exp = jnp.exp(past - highest[..., None])
    own_exp = jnp.exp(self_part - highest)
    denominator = lax.optimization_barrier(jnp.sum(past_exp, axis=-1)) + own_exp
    past_weight = lax.optimization_barrier((past_exp / denominator[..., None]).astype(jnp.bfloat16)).astype(jnp.float32)
    own_weight = lax.optimization_barrier((own_exp / denominator).astype(jnp.bfloat16)).astype(jnp.float32)
    mixed = jnp.einsum('bkgl,blkd->bkgd', past_weight, value_four) + own_weight[..., None] * own_value[:, :, None, :]
    return mixed.reshape(amount, HEADS * HEAD_DIM).astype(jnp.bfloat16)

def expert_mix(settled, expert_gate, expert_up, expert_down, routes, route_weights):
    shards = N_EP // EXPERTS
    part_width = FF_EXPERT // shards
    chosen = routes.reshape(N_EP, SEQ_DEV, TOP)
    shares = route_weights.reshape(N_EP, SEQ_DEV, TOP)
    expert_ids = jnp.arange(EXPERTS, dtype=jnp.int32)
    picked = (chosen[..., None] == expert_ids).astype(jnp.int32)
    hits = lax.optimization_barrier(jnp.sum(picked, axis=2))
    portion = lax.optimization_barrier(jnp.sum(picked.astype(jnp.float32) * shares[..., None], axis=2))
    ranks = jnp.cumsum(hits, axis=1) - hits
    slot_ids = jnp.arange(CAP, dtype=jnp.int32)
    matched = (hits[..., None] * (ranks[..., None] == slot_ids).astype(jnp.int32)).astype(jnp.float32)
    by_source = settled.astype(jnp.float32).reshape(N_EP, SEQ_DEV, D)

    def one_expert(running, expert):
        select = lax.dynamic_index_in_dim(matched, expert, 2, keepdims=False)
        weight_here = lax.dynamic_index_in_dim(portion, expert, 2, keepdims=False)
        slot_rows = jnp.einsum('nsc,nsd->ncd', select, by_source, precision=lax.Precision.HIGHEST)
        slot_rows = slot_rows.reshape(N_EP * CAP, D).astype(jnp.bfloat16)
        gate_cols = lax.dynamic_slice_in_dim(expert_gate, expert * FF_EXPERT, FF_EXPERT, 1)
        up_cols = lax.dynamic_slice_in_dim(expert_up, expert * FF_EXPERT, FF_EXPERT, 1)
        down_rows = lax.dynamic_slice_in_dim(expert_down, expert * FF_EXPERT, FF_EXPERT, 0)
        gate_val = jnp.dot(slot_rows, gate_cols, preferred_element_type=jnp.float32)
        up_val = jnp.dot(slot_rows, up_cols, preferred_element_type=jnp.float32)
        hidden = (jax.nn.silu(gate_val) * up_val).astype(jnp.bfloat16)
        pieces = jnp.einsum('rgf,gfd->rgd', hidden.astype(jnp.float32).reshape(N_EP * CAP, shards, part_width), down_rows.astype(jnp.float32).reshape(shards, part_width, D))
        pieces = lax.optimization_barrier(pieces.astype(jnp.bfloat16)).astype(jnp.float32)
        summed = lax.optimization_barrier(jnp.sum(pieces, axis=1)).reshape(N_EP, CAP, D)
        placed = jnp.einsum('nsc,ncd->nsd', select, summed, precision=lax.Precision.HIGHEST)
        return (running + weight_here[..., None] * placed, None)
    combined, unused = lax.scan(one_expert, jnp.zeros((N_EP, SEQ_DEV, D), jnp.float32), jnp.arange(EXPERTS, dtype=jnp.int32))
    return combined.reshape(N_EP * SEQ_DEV, D)

def reference(tokens, cache_keys, cache_values, cum_gates, lengths, query_weight, key_weight, value_weight, forget_weight, out_weight, norm_gain, norm_bias, dense_gate_weight, dense_up_weight, dense_down_weight, dense_scale, expert_gate_weight, expert_up_weight, expert_down_weight, routes, route_weights):
    query = jnp.dot(tokens, query_weight, preferred_element_type=jnp.float32).astype(jnp.bfloat16)
    new_key = jnp.dot(tokens, key_weight, preferred_element_type=jnp.float32).astype(jnp.bfloat16)
    new_value = jnp.dot(tokens, value_weight, preferred_element_type=jnp.float32).astype(jnp.bfloat16)
    new_gate = jax.nn.log_sigmoid(jnp.dot(tokens, forget_weight, preferred_element_type=jnp.float32))

    def blocks(array):
        return array.reshape((N_EP, SEQ_DEV) + array.shape[1:])
    attended = lax.map(attend_block, (blocks(query), blocks(cache_keys), blocks(cache_values), blocks(cum_gates), blocks(lengths), blocks(new_key), blocks(new_value), blocks(new_gate)))
    attended = attended.reshape(SEQUENCE_COUNT, HEADS * HEAD_DIM)
    projected = jnp.dot(attended, out_weight, preferred_element_type=jnp.float32)
    settled = layer_norm(residual_scale * tokens.astype(jnp.float32) + projected, norm_gain[0], norm_bias[0])
    dense_gate = jnp.dot(settled, dense_gate_weight, preferred_element_type=jnp.float32)
    dense_up = jnp.dot(settled, dense_up_weight, preferred_element_type=jnp.float32)
    dense_hidden = (jax.nn.silu(dense_gate) * dense_up).astype(jnp.bfloat16)
    dense_out = jnp.dot(dense_hidden, dense_down_weight, preferred_element_type=jnp.float32)
    expert_out = expert_mix(settled, expert_gate_weight, expert_up_weight, expert_down_weight, routes, route_weights)
    ffn = expert_out + dense_scale * dense_out
    return layer_norm(residual_scale * settled.astype(jnp.float32) + ffn, norm_gain[1], norm_bias[1])
```

```python
import functools
import jax
import jax.numpy as jnp
from jax import lax
from jax.experimental import pallas as pl
from jax.experimental.pallas import tpu as pltpu
from jax.sharding import PartitionSpec as P

EXPERTS = 8
CAP = 3
MESH = pl.DeviceIdType.MESH

residual_scale = 1.4142135
norm_eps = 1e-05


def layer_norm(values, gain_row, shift_row):
    centre = jnp.mean(values, axis=-1, keepdims=True)
    centred = values - centre
    spread = jnp.mean(centred * centred, axis=-1, keepdims=True)
    return (centred * lax.rsqrt(spread + norm_eps) * gain_row + shift_row).astype(jnp.bfloat16)


def attend(
    heads, kv_count, tokens_ref, query_weight_ref, key_weight_ref, value_weight_ref,
    forget_ref, keys_ref, values_ref, gates_ref, lengths_ref, query_ref, rows_ref, waits, parts,
):
    seqs, model = tokens_ref.shape
    width = key_weight_ref.shape[1]
    head_dim = width // kv_count
    grouped = heads // kv_count
    cache_len = keys_ref.shape[1]
    ratio_value = head_dim ** (-0.5)
    waits["small"]()
    tokens = tokens_ref[...]
    wide = tokens.astype(jnp.float32)
    fresh_gate = jax.nn.log_sigmoid(
        jnp.concatenate(
            [
                jnp.sum(wide * forget_ref[j:j + 1, :].astype(jnp.float32), axis=1, keepdims=True)
                for j in range(kv_count)
            ],
            axis=1,
        )
    )
    waits["keys"]()
    fresh_key = jnp.dot(tokens, key_weight_ref[...], preferred_element_type=jnp.float32)
    fresh_key = fresh_key.astype(jnp.bfloat16).astype(jnp.float32)
    fresh_value = jnp.dot(tokens, value_weight_ref[...], preferred_element_type=jnp.float32)
    fresh_value = fresh_value.astype(jnp.bfloat16).astype(jnp.float32)
    pieces = waits["pieces"]
    piece = model // pieces
    for i in range(pieces):
        waits["query"](i)
        part = jnp.dot(
            tokens, query_weight_ref[:, i * piece:(i + 1) * piece], preferred_element_type=jnp.float32
        ).astype(jnp.bfloat16).astype(jnp.float32)
        for h in range(piece // head_dim):
            head = i * (piece // head_dim) + h
            group = head // grouped
            fields = [jnp.zeros((seqs, head_dim), jnp.float32)] * kv_count
            fields[group] = part[:, h * head_dim:(h + 1) * head_dim]
            query_ref[head * seqs:(head + 1) * seqs, :] = jnp.concatenate(fields, axis=1)
    positions = lax.broadcasted_iota(jnp.int32, (kv_count, cache_len), 1)
    row_group = lax.broadcasted_iota(jnp.int32, (heads, 1), 0) // grouped
    lanes = rows_ref.shape[1]
    share = head_dim // parts
    batch = seqs // waits["batches"]
    for b in range(seqs):
        if b % batch == 0:
            waits["caches"](b // batch)
        length = lengths_ref[:, b:b + 1]
        gates = gates_ref[b]
        latest = jnp.sum(jnp.where(positions == length - 1, gates, 0.0), axis=1, keepdims=True)
        offsets = jnp.where(positions < length, latest - gates, -jnp.inf)
        spread = offsets[0:1] + fresh_gate[b:b + 1, 0:1]
        spread = jnp.broadcast_to(spread, (heads, cache_len))
        for j in range(1, kv_count):
            spread = jnp.where(row_group == j, offsets[j:j + 1] + fresh_gate[b:b + 1, j:j + 1], spread)
        queries = query_ref[pl.ds(b, heads, stride=seqs), :]
        past = lax.dot_general(
            queries.astype(jnp.bfloat16), keys_ref[b], (((1,), (1,)), ((), ())),
            preferred_element_type=jnp.float32,
        )
        past = past * ratio_value + spread
        self_part = ratio_value * jnp.sum(queries * fresh_key[b:b + 1], axis=1, keepdims=True)
        highest = jnp.maximum(jnp.max(past, axis=1, keepdims=True), self_part)
        past_exp = jnp.exp(past - highest)
        own_exp = jnp.exp(self_part - highest)
        denominator = jnp.sum(past_exp, axis=1, keepdims=True) + own_exp
        mixed = jnp.dot(past_exp.astype(jnp.bfloat16), values_ref[b], preferred_element_type=jnp.float32)
        mixed = (mixed + own_exp * fresh_value[b:b + 1]) / denominator
        mixed = jnp.concatenate(
            [
                mixed[j * grouped:(j + 1) * grouped, j * head_dim:(j + 1) * head_dim]
                for j in range(kv_count)
            ],
            axis=0,
        )
        for p in range(parts):
            block = mixed[:, p * share:(p + 1) * share]
            if share < lanes:
                block = jnp.concatenate([block, jnp.zeros((heads, lanes - share), jnp.float32)], axis=1)
            rows_ref[pl.ds(p * seqs + b, heads, stride=parts * seqs), :] = block


def factors_of(count):
    found = [2]
    rest = count // 2
    while rest > 1:
        step = 4 if rest % 4 == 0 else rest
        found.append(step)
        rest //= step
    return found


def orders_of(stages):
    far = list(range(1, stages))
    return [[0] + far, [0] + far[::-1]]


def step_shapes(factors, order, rows, width):
    left = list(range(len(factors)))[::-1]
    shapes = []
    for axis in order:
        left = [other for other in left if other != axis]
        lead = tuple(factors[other] for other in left)
        shapes.append(((factors[axis] - 1,) + lead + (rows, width), lead + (rows, width)))
    return shapes


class Phase:
    now = None


def phase(name):
    return None


def kernel(
    count, factors, orders, widths, heads,
    tokens_hbm, gates_hbm, lengths_hbm, forget_hbm, gain_hbm, bias_hbm, scale_hbm,
    routes_hbm, shares_hbm, query_hbm, key_hbm, value_hbm, keys_hbm, values_hbm, out_hbm,
    gate_hbm, up_hbm, down_hbm, dense_gate_hbm, dense_up_hbm, dense_down_hbm,
    result_ref, *scratch,
):
    pool = list(scratch)
    take = lambda amount: [pool.pop(0) for _ in range(amount)]
    tokens_ref, gates_ref, lengths_ref, forget_ref, gain_ref, bias_ref, scale_ref = take(7)
    routes_ref, shares_ref, small_sem = take(3)
    gate_ref, up_ref, down_ref, dense_gate_ref, dense_up_ref, dense_down_ref, load_sem = take(7)
    query_weight_ref, key_weight_ref, value_weight_ref, keys_ref, values_ref, early_sem = take(6)
    out_weight_ref, out_sem = take(2)
    query_ref, attended_rows_ref, attended_ref, share_ref, pick_ref, place_ref = take(6)
    mixed_ref, mixed_sem, rows_ref, compact_ref, hidden_ref, dense_ref, settled_ref = take(7)
    cross_start, cross_land, cross_mid, cross_far, cross_sem = take(5)
    stages = len(factors)
    chunks = len(orders)
    per_chunk = []
    for c in range(chunks):
        start = take(1)[0]
        lands = take(stages)
        sums = take(stages - 1)
        per_chunk.append((start, lands, sums))
    exchange_sem = take(1)[0]
    gathered = take(chunks)
    gather_sem = take(1)[0]
    total_rows, model = rows_ref.shape
    seqs = tokens_ref.shape[0]

    me = lax.axis_index("ep")
    coords, strides, rest, stride = [], [], me, 1
    for factor in factors:
        coords.append(lax.rem(rest, factor))
        strides.append(stride)
        rest = rest // factor
        stride *= factor

    def partner(axis, k):
        other = lax.rem(coords[axis] + k, factors[axis])
        return other, me + (other - coords[axis]) * strides[axis]

    def remote(source, target, sems, device):
        return pltpu.make_async_remote_copy(
            src_ref=source, dst_ref=target, send_sem=sems[0], recv_sem=sems[1],
            device_id=(device,), device_id_type=MESH,
        )

    far = factors[-1]
    middle = count // (2 * far)
    core, depth = coords[0], coords[-1]
    place_here = lax.rem(me // 2, middle)
    column = 2 * far
    member = depth * 2 + core

    def across(k):
        other = lax.rem(place_here + k, middle)
        return (depth * middle + other) * 2 + core

    def along(k):
        other = lax.rem(member + k, column)
        return other, ((other // 2) * middle + place_here) * 2 + lax.rem(other, 2)

    barrier = pltpu.get_barrier_semaphore()
    peers = [across(k) for k in range(1, middle)] + [along(k)[1] for k in range(1, column)]

    sources = (gate_hbm, up_hbm, down_hbm, dense_gate_hbm, dense_up_hbm, dense_down_hbm)
    targets = (gate_ref, up_ref, down_ref, dense_gate_ref, dense_up_ref, dense_down_ref)
    loads = [
        pltpu.make_async_copy(source, target, load_sem.at[i])
        for i, (source, target) in enumerate(zip(sources, targets))
    ]
    small = [
        pltpu.make_async_copy(source, target, small_sem.at[i])
        for i, (source, target) in enumerate(
            [
                (tokens_hbm, tokens_ref), (forget_hbm, forget_ref), (gates_hbm, gates_ref),
                (lengths_hbm, lengths_ref), (routes_hbm, routes_ref), (shares_hbm, shares_ref),
                (gain_hbm, gain_ref), (bias_hbm, bias_ref), (scale_hbm, scale_ref),
            ]
        )
    ]
    pieces = 4
    piece = model // pieces
    early = [
        pltpu.make_async_copy(source, target, early_sem.at[i])
        for i, (source, target) in enumerate(
            [(key_hbm, key_weight_ref), (value_hbm, value_weight_ref)]
            + [
                (
                    query_hbm.at[:, pl.ds(i * piece, piece)],
                    query_weight_ref.at[:, pl.ds(i * piece, piece)],
                )
                for i in range(pieces)
            ]
        )
    ]
    batches = 2
    batch = seqs // batches
    caches = [
        [
            pltpu.make_async_copy(
                source.at[pl.ds(i * batch, batch)], target.at[pl.ds(i * batch, batch)],
                early_sem.at[2 + pieces + 2 * i + j],
            )
            for j, (source, target) in enumerate([(keys_hbm, keys_ref), (values_hbm, values_ref)])
        ]
        for i in range(batches)
    ]

    def wait_all(some):
        for copy in some:
            copy.wait()

    out_rows = out_hbm.shape[0]
    own_rows = out_weight_ref.at[pl.ds(pl.multiple_of(place_here * out_rows, out_rows), out_rows)]
    own_out = pltpu.make_async_copy(out_hbm, own_rows, out_sem.at[2])

    small[0].start()
    small[1].start()
    for copy in early:
        copy.start()
    for copy in small[2:]:
        copy.start()
    own_out.start()
    for peer in peers:
        pl.semaphore_signal(barrier, inc=1, device_id=(peer,), device_id_type=MESH)
    for i in range(batches):
        for copy in caches[i]:
            copy.start()

    def spread_out_weight():
        phase("barrier")
        pl.semaphore_wait(barrier, len(peers))
        phase("gather")
        for k in range(1, middle):
            remote(out_hbm, own_rows, (out_sem.at[0], out_sem.at[1]), across(k)).start()

    def wait_small():
        phase("small")
        wait_all(small[:2])
        spread_out_weight()
        phase("gate")

    def wait_keys():
        phase("kv_wait")
        wait_all(early[:2])
        phase("kv")

    def wait_query(i):
        phase("q_wait" + str(i))
        early[2 + i].wait()
        phase("query" + str(i))

    def wait_caches(i):
        phase("cache_wait" + str(i))
        if i == 0:
            wait_all(small[2:4])
        wait_all(caches[i])
        if i == batches - 1:
            for load in loads:
                load.start()
        phase("attn" + str(i))

    waits = {
        "small": wait_small, "keys": wait_keys, "query": wait_query,
        "pieces": pieces, "caches": wait_caches, "batches": batches,
    }
    kv_count = gates_ref.shape[1]
    attend(
        heads, kv_count, tokens_ref, query_weight_ref, key_weight_ref, value_weight_ref,
        forget_ref, keys_ref, values_ref, gates_ref, lengths_ref, query_ref,
        attended_rows_ref, waits, count // heads,
    )
    phase("a2a_start")
    for t in range(column):
        blocks = [
            attended_rows_ref[pl.ds((((t // 2) * middle + m) * 2 + t % 2) * seqs, seqs), :][:, :out_rows]
            for m in range(middle)
        ]
        attended_ref[t] = jnp.concatenate(blocks, axis=1).astype(jnp.bfloat16)
    for k in range(1, column):
        other, device = along(k)
        remote(
            attended_ref.at[other], mixed_ref.at[member], (mixed_sem.at[0], mixed_sem.at[1]), device
        ).start()
    mixed_ref[member] = attended_ref[member]

    phase("share")
    wait_all(small[4:])
    own_expert = me // (count // EXPERTS)
    row_tile = min(total_rows, 256)
    tiles = total_rows // row_tile
    blocks_of = row_tile // seqs
    slots = blocks_of * CAP
    row_of = lax.broadcasted_iota(jnp.int32, (row_tile, row_tile), 0)
    column_of = lax.broadcasted_iota(jnp.int32, (row_tile, row_tile), 1)
    before = jnp.where((row_of // seqs == column_of // seqs) & (row_of < column_of), 1.0, 0.0)
    before = before.astype(jnp.bfloat16)
    slot_of = lax.broadcasted_iota(jnp.int32, (slots, row_tile), 0)
    first_of = lax.broadcasted_iota(jnp.int32, (slots, row_tile), 1) // seqs * CAP
    for i in range(tiles):
        at = slice(i * row_tile, (i + 1) * row_tile)
        matches = routes_ref[:, at] == own_expert
        chosen = jnp.sum(jnp.where(matches, shares_ref[:, at], 0.0), axis=0, keepdims=True)
        hits = jnp.sum(jnp.where(matches, 1.0, 0.0), axis=0, keepdims=True)
        rank = jnp.dot(
            jnp.broadcast_to(hits, (8, row_tile)).astype(jnp.bfloat16), before,
            preferred_element_type=jnp.float32,
        )[0:1]
        wanted = first_of + rank.astype(jnp.int32)
        picked = jnp.where((wanted == slot_of) & (hits > 0.5), 1.0, 0.0)
        share_ref[i * slots:(i + 1) * slots, :] = jnp.sum(picked * chosen, axis=1, keepdims=True)
        pick_ref[i * slots:(i + 1) * slots, :] = picked.astype(jnp.bfloat16)
        place_ref[at, :] = picked.T.astype(jnp.bfloat16)

    def wait_bytes(block, sems, device):
        copy = remote(block, block, sems, device)
        copy.wait()

    phase("a2a_wait")
    wait_bytes(
        mixed_ref.at[pl.ds(0, column - 1)], (mixed_sem.at[0], mixed_sem.at[1]), along(1)[1]
    )
    phase("gather_wait")
    own_out.wait()
    if middle > 1:
        wait_bytes(
            out_weight_ref.at[pl.ds(0, (middle - 1) * out_rows)], (out_sem.at[0], out_sem.at[1]),
            across(1),
        )

    phase("proj")
    left_side = mixed_ref[...].astype(jnp.float32).reshape(column * seqs, middle * out_rows)
    left_side = left_side.astype(jnp.bfloat16)
    halves = cross_start.shape[0]
    half = model // halves
    _, twin = partner(0, 1)
    for h in range(halves):
        part = jnp.dot(
            left_side, out_weight_ref[:, h * half:(h + 1) * half], preferred_element_type=jnp.float32
        )
        part = part.reshape(far, 2, seqs, half).astype(jnp.bfloat16)
        for j in range(2):
            cross_start[h, j] = part[:, j]
        remote(
            cross_start.at[h, 1 - core], cross_land.at[h], (cross_sem.at[0, h, 0], cross_sem.at[0, h, 1]),
            twin,
        ).start()
    phase("rs1a")
    for h in range(halves):
        wait_bytes(cross_land.at[h], (cross_sem.at[0, h, 0], cross_sem.at[0, h, 1]), twin)
        summed = cross_start[h, core].astype(jnp.float32) + cross_land[h].astype(jnp.float32)
        cross_mid[h] = summed.astype(jnp.bfloat16)
        for k in range(far - 1, 0, -1):
            other, device = partner(stages - 1, k)
            remote(
                cross_mid.at[h, other], cross_far.at[h, k - 1],
                (cross_sem.at[1, h, 0], cross_sem.at[1, h, 1]), device,
            ).start()
    phase("rs1b")
    projected = []
    for h in range(halves):
        wait_bytes(cross_far.at[h], (cross_sem.at[1, h, 0], cross_sem.at[1, h, 1]), twin)
        own = cross_mid[h, depth].astype(jnp.float32)
        for k in range(far - 1):
            own = own + cross_far[h, k].astype(jnp.float32)
        projected.append(own)
    projected = jnp.concatenate(projected, axis=-1)
    phase("norm1")
    settled = layer_norm(
        residual_scale * tokens_ref[...].astype(jnp.float32) + projected, gain_ref[0:1], bias_ref[0:1]
    )
    settled_ref[...] = settled

    def at_axis(left, axis, index):
        return tuple(index if other == axis else slice(None) for other in left)

    def exchanger():
        current = [entry[0] for entry in per_chunk]
        left = [list(range(stages))[::-1] for _ in orders]
        finished = [None] * chunks

        def sems(c, stage):
            return exchange_sem.at[c, stage, 0], exchange_sem.at[c, stage, 1]

        def launch(c, stage):
            axis = orders[c][stage]
            for k in range(1, factors[axis]):
                other, device = partner(axis, k)
                remote(
                    current[c].at[at_axis(left[c], axis, other)], per_chunk[c][1][stage].at[k - 1],
                    sems(c, stage), device,
                ).start()

        def advance(c, stage):
            axis = orders[c][stage]
            landed = per_chunk[c][1][stage]
            wait_bytes(landed, sems(c, stage), partner(axis, 1)[1])
            own = current[c][at_axis(left[c], axis, coords[axis])].astype(jnp.float32)
            for k in range(factors[axis] - 1):
                own = own + landed[k].astype(jnp.float32)
            left[c] = [other for other in left[c] if other != axis]
            if stage == stages - 1:
                finished[c] = own
            else:
                current[c] = per_chunk[c][2][stage]
                current[c][...] = own.astype(jnp.bfloat16)
                launch(c, stage + 1)

        def finish():
            for stage in range(stages):
                for c in range(chunks):
                    if stage or c:
                        advance(c, stage)
            return jnp.concatenate(finished, axis=-1)

        def computed(c):
            launch(c, 0)
            if c == 1:
                advance(0, 0)

        return computed, finish

    def place(start_ref, first, value, column, span):
        blocks = value.shape[0] // seqs
        lead = start_ref.shape[:-2]
        flat = value.reshape(blocks, seqs, span).astype(jnp.bfloat16)
        inner = lead[1:]
        size = 1
        for factor in inner:
            size *= factor
        whole = blocks // size
        start_ref[pl.ds(first * whole, whole), ..., column] = flat.reshape((whole,) + inner + (seqs, span))

    phase("ag")
    mine = tuple(coords[axis] for axis in range(stages)[::-1])
    begin = 0
    for c in range(chunks):
        gathered[c][mine] = settled[:, begin:begin + widths[c]]
        begin += widths[c]
    have = [[] for _ in orders]

    def gather_sems(c, stage):
        return gather_sem.at[c, stage, 0], gather_sem.at[c, stage, 1]

    def region(c):
        return tuple(
            slice(None) if other in have[c] else coords[other] for other in range(stages)[::-1]
        )

    def spread(c, stage):
        axis = orders[c][::-1][stage]
        block = gathered[c].at[region(c)]
        for k in range(1, factors[axis]):
            _, device = partner(axis, k)
            remote(block, block, gather_sems(c, stage), device).start()

    def arrive(c, stage):
        axis = orders[c][::-1][stage]
        index = tuple(
            pl.ds(0, factors[other] - 1) if other == axis else (slice(None) if other in have[c] else 0)
            for other in range(stages)[::-1]
        )
        wait_bytes(gathered[c].at[index], gather_sems(c, stage), partner(axis, 1)[1])
        have[c].append(axis)

    for c in range(chunks):
        spread(c, 0)
    for stage in range(stages):
        for c in range(chunks):
            arrive(c, stage)
            if stage < stages - 1:
                spread(c, stage + 1)
    phase("rows")
    begin = 0
    for c in range(chunks):
        block = gathered[c][...].astype(jnp.float32).reshape(total_rows, widths[c])
        rows_ref[:, begin:begin + widths[c]] = block.astype(jnp.bfloat16)
        begin += widths[c]

    phase("pick")
    for i in (0, 1, 3, 4):
        loads[i].wait()
    span = 256
    units = gate_ref.shape[1]
    unit_span = span if units % span == 0 else units

    for i in range(tiles):
        compact_ref[i * slots:(i + 1) * slots, :] = jnp.dot(
            pick_ref[i * slots:(i + 1) * slots, :], rows_ref[i * row_tile:(i + 1) * row_tile, :],
            preferred_element_type=jnp.float32,
        ).astype(jnp.bfloat16)

    def hidden_of(inputs, gates, ups, depth=0):
        contract = (((1,), (depth,)), ((), ()))
        gate_val = lax.dot_general(inputs, gates, contract, preferred_element_type=jnp.float32)
        up_val = lax.dot_general(inputs, ups, contract, preferred_element_type=jnp.float32)
        return (jax.nn.silu(gate_val) * up_val).astype(jnp.bfloat16)

    phase("ffn1d")
    for i in range(tiles):
        at_rows = slice(i * row_tile, (i + 1) * row_tile)
        dense_ref[at_rows, :] = hidden_of(rows_ref[at_rows, :], dense_gate_ref[...], dense_up_ref[...], 1)
    phase("ffn1e")
    for step in range(units // unit_span):
        at_units = slice(step * unit_span, (step + 1) * unit_span)
        hidden_ref[:, at_units] = hidden_of(compact_ref[...], gate_ref[:, at_units], up_ref[:, at_units])

    phase("ffn2")
    for i in (2, 5):
        loads[i].wait()
    computed, finish = exchanger()
    begin = 0
    for c in range(chunks):
        for step in range(widths[c] // span):
            at_columns = slice(begin + step * span, begin + (step + 1) * span)
            expert_out = jnp.dot(
                hidden_ref[...], down_ref[:, at_columns], preferred_element_type=jnp.float32
            )
            expert_out = (share_ref[...] * expert_out).astype(jnp.bfloat16)
            for i in range(tiles):
                at_rows = slice(i * row_tile, (i + 1) * row_tile)
                dense_out = jnp.dot(
                    dense_ref[at_rows, :], dense_down_ref[:, at_columns],
                    preferred_element_type=jnp.float32,
                )
                placed = jnp.dot(
                    place_ref[at_rows, :], expert_out[i * slots:(i + 1) * slots],
                    preferred_element_type=jnp.float32,
                )
                part = placed + scale_ref[:, at_columns] * dense_out
                place(per_chunk[c][0], i, part, pl.ds(step * span, span), span)
        begin += widths[c]
        computed(c)

    phase("rs2")
    ffn = finish()
    phase("norm2")
    result_ref[...] = layer_norm(
        residual_scale * settled_ref[...].astype(jnp.float32) + ffn, gain_ref[1:2], bias_ref[1:2]
    )
    phase(None)


def whole_step(
    count, heads, tokens, gates, lengths, forget, norm_gain, norm_bias, dense_scale, routes, shares,
    query_weight, key_weight, value_weight, cache_keys, cache_values, out_weight,
    expert_gate, expert_up, expert_down, dense_gate, dense_up, dense_down,
):
    seqs, model = tokens.shape
    factors = factors_of(count)
    stages = len(factors)
    orders = orders_of(stages)
    chunks = len(orders)
    narrow = model * 3 // 8
    widths = [model - narrow, narrow]
    total_rows = count * seqs
    lead = tuple(factors[::-1])
    far = factors[-1]
    column = 2 * far
    middle = count // column
    out_rows = out_weight.shape[0]
    row_tile = min(total_rows, 256)
    slots = row_tile // seqs * CAP
    tiles = total_rows // row_tile
    halves = 2
    small = (tokens, gates, lengths, forget, norm_gain, norm_bias, dense_scale, routes, shares)
    scratch = [pltpu.VMEM(array.shape, array.dtype) for array in small]
    scratch += [pltpu.SemaphoreType.DMA((len(small),))]
    scratch += [
        pltpu.VMEM(array.shape, array.dtype)
        for array in (expert_gate, expert_up, expert_down, dense_gate, dense_up, dense_down)
    ]
    scratch += [
        pltpu.SemaphoreType.DMA((6,)),
        *[
            pltpu.VMEM(array.shape, array.dtype)
            for array in (query_weight, key_weight, value_weight, cache_keys, cache_values)
        ],
        pltpu.SemaphoreType.DMA((10,)),
        pltpu.VMEM((middle * out_rows, model), jnp.bfloat16),
        pltpu.SemaphoreType.DMA((3,)),
        pltpu.VMEM((heads * seqs, key_weight.shape[1]), jnp.float32),
        pltpu.VMEM((total_rows, 128), jnp.float32),
        pltpu.VMEM((column, seqs, middle * out_rows), jnp.bfloat16),
        pltpu.VMEM((tiles * slots, 1), jnp.float32),
        pltpu.VMEM((tiles * slots, row_tile), jnp.bfloat16),
        pltpu.VMEM((total_rows, slots), jnp.bfloat16),
        pltpu.VMEM((column, seqs, middle * out_rows), jnp.bfloat16),
        pltpu.SemaphoreType.DMA((2,)),
        pltpu.VMEM((total_rows, model), jnp.bfloat16),
        pltpu.VMEM((tiles * slots, model), jnp.bfloat16),
        pltpu.VMEM((tiles * slots, expert_gate.shape[1]), jnp.bfloat16),
        pltpu.VMEM((total_rows, dense_gate.shape[0]), jnp.bfloat16),
        pltpu.VMEM((seqs, model), jnp.bfloat16),
        pltpu.VMEM((halves, 2, far, seqs, model // halves), jnp.bfloat16),
        pltpu.VMEM((halves, far, seqs, model // halves), jnp.bfloat16),
        pltpu.VMEM((halves, far, seqs, model // halves), jnp.bfloat16),
        pltpu.VMEM((halves, far - 1, seqs, model // halves), jnp.bfloat16),
        pltpu.SemaphoreType.DMA((2, halves, 2)),
    ]
    for order, width in zip(orders, widths):
        shapes = step_shapes(factors, order, seqs, width)
        scratch.append(pltpu.VMEM(lead + (seqs, width), jnp.bfloat16))
        scratch += [pltpu.VMEM(shape[0], jnp.bfloat16) for shape in shapes]
        scratch += [pltpu.VMEM(shape[1], jnp.bfloat16) for shape in shapes[:-1]]
    scratch += [pltpu.SemaphoreType.DMA((chunks, stages, 2))]
    scratch += [pltpu.VMEM(lead + (seqs, width), jnp.bfloat16) for width in widths]
    scratch += [pltpu.SemaphoreType.DMA((chunks, stages, 2))]
    away = pl.BlockSpec(memory_space=pl.ANY)
    return pl.pallas_call(
        functools.partial(kernel, count, factors, orders, widths, heads),
        out_shape=pltpu.VMEM((seqs, model), jnp.bfloat16),
        in_specs=[away] * 21,
        out_specs=pl.BlockSpec(memory_space=pltpu.VMEM),
        scratch_shapes=scratch,
        compiler_params=pltpu.CompilerParams(
            collective_id=0, has_side_effects=True, vmem_limit_bytes=60 * 1024 * 1024
        ),
        name="whole_step",
    )(
        tokens, gates, lengths, forget, norm_gain, norm_bias, dense_scale, routes, shares,
        query_weight, key_weight, value_weight, cache_keys, cache_values, out_weight,
        expert_gate, expert_up, expert_down, dense_gate, dense_up, dense_down,
    )


def local(
    tokens,
    cache_keys,
    cache_values,
    cum_gates,
    lengths,
    query_weight,
    key_weight,
    value_weight,
    forget_weight,
    out_weight,
    norm_gain,
    norm_bias,
    dense_gate_weight,
    dense_up_weight,
    dense_down_weight,
    dense_scale,
    expert_gate_weight,
    expert_up_weight,
    expert_down_weight,
    routes,
    route_weights,
):
    count = lax.axis_size("ep")
    head_dim = key_weight.shape[1] // cum_gates.shape[2]
    heads = query_weight.shape[1] // head_dim
    return whole_step(
        count, heads, tokens, jnp.transpose(cum_gates, (0, 2, 1)), lengths[None, :], forget_weight.T,
        norm_gain, norm_bias, dense_scale[None, :], routes.T, route_weights.T,
        query_weight, key_weight, value_weight, cache_keys, cache_values, out_weight,
        expert_gate_weight, expert_up_weight, expert_down_weight,
        dense_gate_weight.T, dense_up_weight.T, dense_down_weight,
    )


def solution(mesh):
    return jax.shard_map(
        local,
        mesh=mesh,
        in_specs=(
            P("ep", None),
            P("ep", None, None),
            P("ep", None, None),
            P("ep", None, None),
            P("ep"),
            P(),
            P(),
            P(),
            P(),
            P("ep", None),
            P(),
            P(),
            P(None, "ep"),
            P(None, "ep"),
            P("ep", None),
            P(),
            P(None, "ep"),
            P(None, "ep"),
            P("ep", None),
            P(),
            P(),
        ),
        out_specs=P("ep", None),
        check_vma=False,
    )
```
